32 devices in a mesh: sp: 16 (over z, y, x), tp: 2 (over core).
Axes of the slice: x: 2, y: 2, z: 4, core: 2. Of those that a mesh axis runs over, the one named last changes fastest.
Arguments:
- queries: bfloat16 [4096, 1024], P('sp', 'tp'), may hold values from -6 to 6
- keys: bfloat16 [4096, 1024], P('sp', 'tp'), may hold values from -6 to 6
- values: bfloat16 [4096, 1024], P('sp', 'tp'), may hold values from -6 to 6
- lambdas: float32 [8], P('tp'), may hold values from 0.3 to 0.8
- head_gain: float32 [128], replicated, may hold values from 0.1 to 1.9
- out_weight: bfloat16 [1024, 2048], P('tp'), may hold values from -0.1875 to 0.1875
- residual: bfloat16 [4096, 2048], P(('sp', 'tp')), may hold values from -6 to 6
- mix_gain: float32 [2048], replicated, may hold values from 0.1 to 1.9
- pre_gain: float32 [2048], replicated, may hold values from 0.1 to 1.9
- gate_weight: bfloat16 [2048, 2816], P('sp', 'tp'), may hold values from -0.125 to 0.125
- up_weight: bfloat16 [2048, 2816], P('sp', 'tp'), may hold values from -0.125 to 0.125
- down_weight: bfloat16 [2048, 2816], P('sp', 'tp'), may hold values from -0.109375 to 0.109375
- ffn_gain: float32 [2048], replicated, may hold values from 0.1 to 1.9
Outputs:
- result: bfloat16 [4096, 2048], P(('sp', 'tp'))
The draws below stay inside these ranges and needn't reach their ends.
All inputs are finite; a program needn't handle non-finite values.
Results may differ from the reference program's by a relative error of at most 0.02.
Values may be sent and summed in bfloat16 or wider, within the bound.
A program may use at most 64 MiB of HBM per device.

```python
import math
import jax
import jax.numpy as jnp
from jax import lax

D = 2048
HEADS = 8
KD = 64
VD = 128
FF = 2816
TOKENS = 4096
N_TP = 2


def drawn(key):
    return jnp.clip(1.3 * jax.random.normal(key, (TOKENS, HEADS, 2, KD), jnp.float32), -6.0, 6.0)


def draw_queries(key, part):
    grid = drawn(jax.random.fold_in(key, 1))
    return grid.reshape(TOKENS, HEADS * 2 * KD).astype(jnp.bfloat16)


def draw_keys(key, part):
    grid = drawn(jax.random.fold_in(key, 2))
    return grid.reshape(TOKENS, HEADS * 2 * KD).astype(jnp.bfloat16)


def steps_of(own_key, shape, cuts, least, largest):
    loudness, own = 1.0, jax.random.fold_in(own_key, 6)
    for position, shards_of in cuts:
        heights = jnp.exp(jax.random.uniform(jax.random.fold_in(own, position), (shards_of,), jnp.float32, least / len(cuts), largest / len(cuts)))
        loudness = loudness * jnp.repeat(heights, shape[position] // shards_of).reshape([-1 if axis == position else 1 for axis in range(len(shape))])
    return loudness


def bell_draw(stream_key, shape, scale, reach, pieces=(), kind=jnp.bfloat16):
    result = jax.random.normal(stream_key, shape, jnp.float32) * scale
    if len(pieces) > 0:
        result = steps_of(stream_key, shape, pieces, -0.22, 0.18) * result
    return jnp.clip(result, min=-reach, max=reach).astype(kind)


def setup_inputs(seed: int = 0) -> dict:
    splits = jax.random.split(jax.random.key(seed), 14)
    return {
        "queries": draw_queries(jax.random.fold_in(splits[13], 71), 0),
        "keys": draw_keys(jax.random.fold_in(splits[13], 71), 0),
        "values": bell_draw(splits[2], (TOKENS, HEADS * VD), 1.0, 6.0, ((0, 16), (1, 2))),
        "lambdas": jnp.clip(0.3 + 0.5 * jax.random.uniform(splits[3], (HEADS,), jnp.float32) ** steps_of(splits[3], (HEADS,), ((0, 2),), -0.2, 0.2), 0.3, 0.8),
        "head_gain": jnp.clip(1.0 + 0.18 * jax.random.normal(splits[4], (VD,), jnp.float32), 0.1, 1.9),
        "out_weight": bell_draw(splits[5], (HEADS * VD, D), (HEADS * VD) ** -0.5, 0.1875, ((0, 2),)),
        "residual": bell_draw(splits[6], (TOKENS, D), 1.0, 6.0, ((0, 32),)),
        "mix_gain": jnp.clip(1.0 + 0.18 * jax.random.normal(splits[7], (D,), jnp.float32), 0.1, 1.9),
        "pre_gain": jnp.clip(1.0 + 0.18 * jax.random.normal(splits[8], (D,), jnp.float32), 0.1, 1.9),
        "gate_weight": bell_draw(splits[9], (D, FF), D ** -0.5, 0.125, ((0, 16), (1, 2))),
        "up_weight": bell_draw(splits[10], (D, FF), D ** -0.5, 0.125, ((0, 16), (1, 2))),
        "down_weight": bell_draw(splits[11], (D, FF), FF ** -0.5, 0.109375, ((0, 16), (1, 2))),
        "ffn_gain": jnp.clip(1.0 + 0.18 * jax.random.normal(splits[12], (D,), jnp.float32), 0.1, 1.9),
    }


epsilon = 1e-06

def normalize(matrix, gain):
    return matrix * lax.rsqrt(lax.optimization_barrier(jnp.mean(matrix * matrix, axis=-1, keepdims=True)) + epsilon) * gain

def rounded(matrix):
    return lax.optimization_barrier(matrix.astype(jnp.bfloat16)).astype(jnp.float32)

def reference(queries, keys, values, lambdas, head_gain, out_weight, residual, mix_gain, pre_gain, gate_weight, up_weight, down_weight, ffn_gain):
    query_grid = queries.reshape(TOKENS, HEADS, 2, KD)
    key_grid = keys.reshape(TOKENS, HEADS, 2, KD)
    value_grid = values.reshape(TOKENS, HEADS, VD)
    block = math.gcd(TOKENS, 1024)
    blocks = TOKENS // block
    positions = jnp.arange(TOKENS, dtype=jnp.int32)
    scale = 1.0 / math.sqrt(KD)

    def one_block(pair):
        head, number = pair
        query_head = lax.dynamic_index_in_dim(query_grid, head, 1, keepdims=False)
        key_head = lax.dynamic_index_in_dim(key_grid, head, 1, keepdims=False)
        value_head = lax.dynamic_index_in_dim(value_grid, head, 1, keepdims=False)
        query_block = lax.dynamic_slice_in_dim(query_head, number * block, block, 0)
        scores = jnp.einsum('rcd,ncd->crn', query_block.astype(jnp.float32), key_head.astype(jnp.float32)) * scale
        query_pos = number * block + jnp.arange(block, dtype=jnp.int32)
        visible = positions[None, :] <= query_pos[:, None]
        row_max = lax.optimization_barrier(jnp.max(jnp.where(visible, scores, -jnp.inf), axis=-1, keepdims=True))
        expo = jnp.where(visible, jnp.exp(scores - row_max), 0.0)
        totals = lax.optimization_barrier(jnp.sum(expo, axis=-1))
        expo_rounded = rounded(expo)
        accum = jnp.einsum('crn,ne->cre', expo_rounded, value_head.astype(jnp.float32))
        ratio = accum / totals[..., None]
        attended = ratio[0] - lambdas[head] * ratio[1]
        return normalize(attended, head_gain).astype(jnp.bfloat16)
    head_index = jnp.repeat(jnp.arange(HEADS, dtype=jnp.int32), blocks)
    block_index = jnp.tile(jnp.arange(blocks, dtype=jnp.int32), HEADS)
    outputs = lax.map(one_block, (head_index, block_index))
    head_out = jnp.transpose(outputs.reshape(HEADS, TOKENS, VD), (1, 0, 2)).reshape(TOKENS, HEADS * VD)
    group = HEADS // N_TP * VD
    projected = jnp.zeros((TOKENS, D), jnp.float32)
    for index in range(N_TP):
        piece_sum = jnp.dot(head_out[:, index * group:(index + 1) * group], out_weight[index * group:(index + 1) * group], preferred_element_type=jnp.float32)
        projected = projected + rounded(piece_sum)
    mixed = (residual.astype(jnp.float32) + normalize(projected, mix_gain)).astype(jnp.bfloat16)
    normed = normalize(mixed.astype(jnp.float32), pre_gain).astype(jnp.bfloat16)
    gate = jnp.dot(normed, gate_weight, preferred_element_type=jnp.float32)
    upward = jnp.dot(normed, up_weight, preferred_element_type=jnp.float32)
    hidden = (jax.nn.silu(gate) * upward).astype(jnp.bfloat16)
    width = FF // N_TP
    ffn_out = jnp.zeros((TOKENS, D), jnp.float32)
    for index in range(N_TP):
        piece_sum = lax.dot_general(hidden[:, index * width:(index + 1) * width], down_weight[:, index * width:(index + 1) * width], (((1,), (1,)), ((), ())), preferred_element_type=jnp.float32)
        ffn_out = ffn_out + rounded(piece_sum)
    return (mixed.astype(jnp.float32) + normalize(ffn_out, ffn_gain)).astype(jnp.bfloat16)
```

```python
import functools
import math

import jax
import jax.numpy as jnp
from jax import lax
from jax.experimental import pallas as pl
from jax.experimental.pallas import tpu as pltpu
from jax.sharding import PartitionSpec as P

KD = 64
VD = 128


epsilon = 1e-06
negative = -1e30


def normalize(matrix, gain):
    return matrix * lax.rsqrt(jnp.mean(matrix * matrix, axis=-1, keepdims=True) + epsilon) * gain


def rounded(matrix):
    return lax.optimization_barrier(matrix.astype(jnp.bfloat16)).astype(jnp.float32)


def on_device(
    queries,
    keys,
    values,
    lambdas,
    head_gain,
    out_weight,
    residual,
    mix_gain,
    pre_gain,
    gate_weight,
    up_weight,
    down_weight,
    ffn_gain,
):
    rows = queries.shape[0]
    heads_dev = values.shape[1] // VD
    offset = lax.axis_index("sp") * rows
    scale = 1.0 / math.sqrt(KD)
    groups = [(queries, offset + jnp.arange(rows, dtype=jnp.int32))]
    grids = [
        (group_rows.reshape(group_rows.shape[0], heads_dev, 2, KD), group_pos)
        for group_rows, group_pos in groups
    ]
    initial = tuple(
        (
            (
                jnp.full((heads_dev, 2, grid.shape[0]), negative, jnp.float32),
                jnp.zeros((heads_dev, 2, grid.shape[0]), jnp.float32),
                jnp.zeros((heads_dev, 2, grid.shape[0], VD), jnp.float32),
            )
            for grid, _ in grids
        )
    )
    key_piece = lax.all_gather(keys, "sp", axis=0, tiled=True)
    value_piece = lax.all_gather(values, "sp", axis=0, tiled=True)
    count = key_piece.shape[0]
    block = math.gcd(count, max(256, 2048 // heads_dev))
    key_grid = key_piece.reshape(count, heads_dev, 2, KD)
    value_grid = value_piece.reshape(count, heads_dev, VD)
    results = []
    for (query_grid, query_pos), carried_group in zip(grids, initial):
        last_pos = query_pos[-1]

        def visit(index, carried, query_grid=query_grid, query_pos=query_pos, last_pos=last_pos):
            first = index * block

            def update(current):
                maxima, totals, accum = current
                key_block = lax.dynamic_slice_in_dim(key_grid, first, block, 0)
                value_block = lax.dynamic_slice_in_dim(value_grid, first, block, 0)
                scores = (
                    jnp.einsum(
                        "rhcd,nhcd->hcrn", query_grid, key_block, preferred_element_type=jnp.float32
                    )
                    * scale
                )
                key_pos = first + jnp.arange(block, dtype=jnp.int32)
                visible = key_pos[None, :] <= query_pos[:, None]
                block_max = jnp.max(jnp.where(visible, scores, negative), axis=-1)
                new_max = jnp.maximum(maxima, block_max)
                weights = jnp.where(visible, jnp.exp(scores - new_max[..., None]), 0.0)
                factor = jnp.exp(maxima - new_max)
                totals = totals * factor + jnp.sum(weights, axis=-1)
                accum = accum * factor[..., None] + jnp.einsum(
                    "hcrn,nhe->hcre",
                    weights.astype(jnp.bfloat16),
                    value_block,
                    preferred_element_type=jnp.float32,
                )
                return (new_max, totals, accum)

            return lax.cond(first <= last_pos, update, lambda current: current, carried)

        results.append(lax.fori_loop(0, count // block, visit, carried_group))
    states = tuple(results)
    totals = jnp.concatenate([state[1] for state in states], axis=2)
    accum = jnp.concatenate([state[2] for state in states], axis=2)
    ratio = accum / totals[..., None]
    attended = ratio[:, 0] - lambdas[:, None, None] * ratio[:, 1]
    heads_normed = normalize(attended, head_gain).astype(jnp.bfloat16)
    head_out = jnp.transpose(heads_normed, (1, 0, 2)).reshape(rows, heads_dev * VD)
    section = head_out
    projected = lax.psum_scatter(
        rounded(jnp.dot(section, out_weight, preferred_element_type=jnp.float32)).astype(
            jnp.bfloat16
        ),
        "tp",
        scatter_dimension=0,
        tiled=True,
    ).astype(jnp.float32)
    mixed = (residual.astype(jnp.float32) + normalize(projected, mix_gain)).astype(jnp.bfloat16)
    normed = normalize(mixed.astype(jnp.float32), pre_gain).astype(jnp.bfloat16)
    inputs = lax.all_gather(normed, "tp", axis=0, tiled=True)
    gate_sum = jnp.dot(
        inputs,
        lax.all_gather(gate_weight, "sp", axis=0, tiled=True),
        preferred_element_type=jnp.float32,
    )
    up_sum = jnp.dot(
        inputs,
        lax.all_gather(up_weight, "sp", axis=0, tiled=True),
        preferred_element_type=jnp.float32,
    )
    down_rows = lax.all_gather(down_weight, "sp", axis=0, tiled=True)
    hidden = (jax.nn.silu(gate_sum) * up_sum).astype(jnp.bfloat16)
    section = hidden
    ffn_out = lax.psum_scatter(
        rounded(
            lax.dot_general(
                section, down_rows, (((1,), (1,)), ((), ())), preferred_element_type=jnp.float32
            )
        ).astype(jnp.bfloat16),
        "tp",
        scatter_dimension=0,
        tiled=True,
    ).astype(jnp.float32)
    return (mixed.astype(jnp.float32) + normalize(ffn_out, ffn_gain)).astype(jnp.bfloat16)


MESH = pl.DeviceIdType.MESH
QUAD = 4
F32 = jnp.float32
BF16 = jnp.bfloat16


def nt_dot(a, b):
    return lax.dot_general(a, b, (((1,), (1,)), ((), ())), preferred_element_type=F32)


def tn_dot(a, b):
    return lax.dot_general(a, b, (((0,), (0,)), ((), ())), preferred_element_type=F32)


def rms(matrix):
    return matrix * lax.rsqrt(jnp.mean(matrix * matrix, axis=-1, keepdims=True) + epsilon)


def layer_kernel(
    q_ref, k_ref, v_ref, lam_ref, hgain_ref, ow_ref, res_ref, mgain_ref, pgain_ref,
    gw_ref, uw_ref, dw_ref, fgain_ref, out_ref,
    qbuf, kbuf, vbuf, gbuf, ubuf, dbuf, qz, m_st, l_st, acc_st, hs, ho,
    ptx, prx, mixed, xbuf, pbuf, ftx, frx, fown, rtx, rrx,
    send, recv, local,
):
    rows = q_ref.shape[0]
    half = rows // 2
    wrows = gw_ref.shape[0]
    width = gbuf.shape[1]
    lanes = 128
    blocks = gw_ref.shape[1] // lanes
    per = width // lanes
    s = lax.axis_index("sp")
    c = lax.axis_index("tp")
    k = s // 8
    q = (s // 2) % 4
    x = s % 2
    zl, y = q // 2, q % 2

    def peer(d):
        return (zl if d < 2 else 1 - zl) * 2 + (y if d % 2 == 0 else 1 - y)

    def chip(kk, qq, xx):
        return kk * 8 + qq * 2 + xx

    sib = 1 - c
    qs = [peer(d) for d in range(4)]
    quad_dev = [(chip(k, qs[d], x), c) for d in range(4)]
    x_dev = (chip(k, q, 1 - x), c)
    k_dev = (chip(1 - k, q, x), c)
    sib_dev = (s, sib)

    barrier = pltpu.get_barrier_semaphore()
    partners = quad_dev[1:] + [x_dev, k_dev, sib_dev]
    for dev in partners:
        pl.semaphore_signal(barrier, inc=1, device_id=dev, device_id_type=MESH)
    pl.semaphore_wait(barrier, len(partners))

    def rc(src, dst, i, dev):
        return pltpu.make_async_remote_copy(
            src_ref=src, dst_ref=dst, send_sem=send.at[i], recv_sem=recv.at[i],
            device_id=dev, device_id_type=MESH,
        )

    def head_cols(qq):
        return pl.ds(pl.multiple_of(qq * lanes, lanes), lanes)

    def unit_start(qq):
        return jnp.minimum(qq * per, blocks - per)

    def unit_cols(qq):
        return pl.ds(pl.multiple_of(unit_start(qq) * lanes, lanes), width)

    def kv_rows(ss):
        return pl.ds(pl.multiple_of(ss * rows, rows), rows)

    def w_rows(ss):
        return pl.ds(pl.multiple_of(ss * wrows, wrows), wrows)

    started = []

    def go(copy):
        copy.start()
        started.append(copy)

    me = s
    kv = [kbuf, vbuf]
    ws = [gbuf, ubuf, dbuf]
    own = []
    for i, (src, dst, at, cols) in enumerate(
        [
            (q_ref, qbuf, kv_rows(q), head_cols(q)),
            (k_ref, kbuf, kv_rows(me), head_cols(q)),
            (v_ref, vbuf, kv_rows(me), head_cols(q)),
            (gw_ref, gbuf, w_rows(me), unit_cols(q)),
            (uw_ref, ubuf, w_rows(me), unit_cols(q)),
            (dw_ref, dbuf, w_rows(me), unit_cols(q)),
        ]
    ):
        cp = pltpu.make_async_copy(src.at[:, cols], dst.at[at, :], local.at[i])
        cp.start()
        own.append(cp)
    for d in (1, 2, 3):
        for a, (src, dst) in enumerate([(k_ref, kbuf), (v_ref, vbuf), (q_ref, qbuf)]):
            slot = dst.at[kv_rows(me if a < 2 else q), :]
            go(rc(src.at[:, head_cols(qs[d])], slot, (d - 1) * 6 + a, quad_dev[d]))
    for d in (1, 2, 3):
        for a, (src, dst) in enumerate([(gw_ref, gbuf), (uw_ref, ubuf), (dw_ref, dbuf)]):
            go(rc(src.at[:, unit_cols(qs[d])], dst.at[w_rows(me), :], (d - 1) * 6 + 3 + a, quad_dev[d]))
    for cp in own:
        cp.wait()

    X0, K0, R0 = 18, 38, 58
    kv_cond = []

    def kslot(a, ss):
        return kv[a].at[kv_rows(ss), :]

    def wslot(a, ss):
        return ws[a].at[w_rows(ss), :]

    for d in range(4):
        ss = chip(k, qs[d], x)
        for a in range(2):
            slot = kslot(a, ss)
            if d > 0:
                rc(slot, slot, (d - 1) * 6 + a, quad_dev[d]).wait_recv()
            go(rc(slot, slot, X0 + d * 5 + a, x_dev))
            copy = rc(slot, slot, K0 + d * 5 + a, k_dev)
            kv_cond.append(copy)

            @pl.when(k == 0)
            def _(copy=copy):
                copy.start()

    for d in range(4):
        ss = chip(k, qs[d], x)
        for a in range(3):
            slot = wslot(a, ss)
            if d > 0:
                rc(slot, slot, (d - 1) * 6 + 3 + a, quad_dev[d]).wait_recv()
            go(rc(slot, slot, K0 + d * 5 + 2 + a, k_dev))
            go(rc(slot, slot, X0 + d * 5 + 2 + a, x_dev))
    for d in (1, 2, 3):
        slot = qbuf.at[kv_rows(qs[d]), :]
        rc(slot, slot, (d - 1) * 6 + 2, quad_dev[d]).wait_recv()
    for d in range(4):
        for a in range(2):
            slot = kslot(a, chip(k, qs[d], 1 - x))
            rc(slot, slot, X0 + d * 5 + a, x_dev).wait_recv()

    span = 2 * rows
    lane = lax.broadcasted_iota(jnp.int32, (rows, lanes), 1)
    for j in range(4):
        piece = qbuf[j * rows : (j + 1) * rows, :].astype(F32) * (1.0 / math.sqrt(KD))
        qz[j, :rows, :] = jnp.where(lane < KD, piece, 0.0).astype(BF16)
        qz[j, rows:, :] = jnp.where(lane < KD, 0.0, piece).astype(BF16)

    def pair_rows(p):
        return pl.ds(pl.multiple_of(p * span, span), span)

    def update(j, p, carry):
        m, l, acc = carry
        sc = nt_dot(kbuf[pair_rows(p), :], qz[j])
        new = jnp.maximum(m, jnp.max(sc, axis=0, keepdims=True))
        e = jnp.exp(sc - new)
        f = jnp.exp(m - new)
        l = l * f + jnp.sum(e, axis=0, keepdims=True)
        acc = acc * f + tn_dot(vbuf[pair_rows(p), :], e.astype(BF16))
        return new, l, acc

    def chunk_a(j, _):
        p = 4 * k + j
        sc = nt_dot(kbuf[pair_rows(p), :], qz[j])
        key_pos = lax.broadcasted_iota(jnp.int32, sc.shape, 0)
        query_pos = x * rows + lax.broadcasted_iota(jnp.int32, sc.shape, 1) % rows
        sc = jnp.where(key_pos <= query_pos, sc, negative)
        m = jnp.max(sc, axis=0, keepdims=True)
        e = jnp.exp(sc - m)
        l = jnp.sum(e, axis=0, keepdims=True)
        acc = tn_dot(vbuf[pair_rows(p), :], e.astype(BF16))
        m, l, acc = lax.fori_loop(0, j, lambda i, carry: update(j, 4 * k + i, carry), (m, l, acc))
        m_st[j], l_st[j], acc_st[j] = m, l, acc
        return 0

    lax.fori_loop(0, 4, chunk_a, 0)

    relays = []
    for d in range(4):
        for a in range(2):
            slot = kslot(a, chip(1 - k, qs[d], x))
            relays.append(rc(slot, slot, R0 + d * 5 + a, x_dev))

    @pl.when(k == 1)
    def _():
        for d in range(4):
            for a in range(2):
                slot = kslot(a, chip(1 - k, qs[d], x))
                rc(slot, slot, K0 + d * 5 + a, k_dev).wait_recv()
                relays[d * 2 + a].start()
        for d in range(4):
            for a in range(2):
                slot = kslot(a, chip(1 - k, qs[d], 1 - x))
                rc(slot, slot, R0 + d * 5 + a, x_dev).wait_recv()

        def chunk_b(j, _):
            carry = lax.fori_loop(
                0, 4, lambda i, carry: update(j, i, carry), (m_st[j], l_st[j], acc_st[j])
            )
            m_st[j], l_st[j], acc_st[j] = carry
            return 0

        lax.fori_loop(0, 4, chunk_b, 0)

    lam = lam_ref[q]

    def finish(j, _):
        ratio = acc_st[j] / l_st[j]
        att = (ratio[:, :rows] - lam * ratio[:, rows:]).T
        hs[j] = (rms(att) * hgain_ref[...]).astype(BF16)
        return 0

    lax.fori_loop(0, 4, finish, 0)
    H0 = 78
    for d in (3, 1, 2):
        go(rc(hs.at[qs[d]], ho.at[q], H0 + d - 1, quad_dev[d]))
    ho[q] = hs[q]
    for d in (1, 2, 3):
        rc(ho.at[qs[d]], ho.at[qs[d]], H0 + d - 1, quad_dev[d]).wait_recv()

    def head_rows(cc):
        at = pl.ds(pl.multiple_of(cc * half, half), half)
        return jnp.concatenate([ho[j, at, :] for j in range(4)], axis=1)

    theirs = head_rows(sib)
    ptx[...] = jnp.dot(theirs, ow_ref[...], preferred_element_type=F32).astype(BF16)
    P0 = 81
    go(rc(ptx, prx, P0, sib_dev))
    mixed[...] = jnp.dot(head_rows(c), ow_ref[...], preferred_element_type=F32)
    rc(prx, prx, P0, sib_dev).wait_recv()

    strip = 16

    def mix(i, _):
        at = pl.ds(pl.multiple_of(i * strip, strip), strip)
        total = mixed[at, :].astype(BF16).astype(F32) + prx[at, :].astype(F32)
        mx = (res_ref[at, :].astype(F32) + rms(total) * mgain_ref[...]).astype(BF16).astype(F32)
        mixed[at, :] = mx
        xbuf[q, pl.ds(pl.multiple_of(c * half + i * strip, strip), strip), :] = (
            rms(mx) * pgain_ref[...]
        ).astype(BF16)
        return 0

    lax.fori_loop(0, half // strip, mix, 0)

    A0, S0 = 82, 85
    core_rows = [pl.ds(pl.multiple_of(cc * half, half), half) for cc in (c, sib)]
    mine = xbuf.at[q, core_rows[0], :]
    for d in (3, 1, 2):
        go(rc(mine, mine, A0 + d - 1, quad_dev[d]))
    go(rc(mine, mine, S0, sib_dev))

    for d in range(4):
        for a in range(3):
            slot = wslot(a, chip(1 - k, qs[d], x))
            rc(slot, slot, K0 + d * 5 + 2 + a, k_dev).wait_recv()
            go(rc(slot, slot, R0 + d * 5 + 2 + a, x_dev))
    for d in (1, 2, 3):
        slot = xbuf.at[qs[d], core_rows[0], :]
        rc(slot, slot, A0 + d - 1, quad_dev[d]).wait_recv()
        go(rc(slot, slot, S0 + d, sib_dev))
    for a in range(3):
        for d in range(4):
            slot = wslot(a, chip(k, qs[d], 1 - x))
            rc(slot, slot, X0 + d * 5 + 2 + a, x_dev).wait_recv()
        for d in range(4):
            slot = wslot(a, chip(1 - k, qs[d], 1 - x))
            rc(slot, slot, R0 + d * 5 + 2 + a, x_dev).wait_recv()

    F0, C0 = 89, 93
    fresh = (q * per - unit_start(q)) * lanes
    unit = lax.broadcasted_iota(jnp.int32, (rows, width), 1)

    def summed(d):
        slot = frx.at[d]
        rc(slot, slot, F0 + d, sib_dev).wait_recv()
        total = fown[d].astype(F32) + frx[d].astype(F32)
        if d == 0:
            fown[0] = total.astype(BF16)
        else:
            rtx[d - 1] = total.astype(BF16)
            go(rc(rtx.at[d - 1], rrx.at[d - 1], C0 + d - 1, quad_dev[d]))

    order = (3, 1, 2, 0)
    for n, d in enumerate(order):
        slot = xbuf.at[qs[d], core_rows[1], :]
        rc(slot, slot, S0 + d, sib_dev).wait_recv()
        rows_in = xbuf[qs[d]]
        gate = jnp.dot(rows_in, gbuf[...], preferred_element_type=F32)
        up = jnp.dot(rows_in, ubuf[...], preferred_element_type=F32)
        hid = gate / (1.0 + jnp.exp(-gate)) * up
        hid = jnp.where(unit >= fresh, hid, 0.0).astype(BF16)
        pbuf[...] = nt_dot(hid, dbuf[...]).astype(BF16)
        ftx[d] = pbuf[core_rows[1], :]
        fown[d] = pbuf[core_rows[0], :]
        go(rc(ftx.at[d], frx.at[d], F0 + d, sib_dev))
        if n > 0:
            summed(order[n - 1])
    summed(order[-1])
    for d in (1, 2, 3):
        slot = rrx.at[d - 1]
        rc(slot, slot, C0 + d - 1, quad_dev[d]).wait_recv()

    def last(i, _):
        at = pl.ds(pl.multiple_of(i * strip, strip), strip)
        total = fown[0, at, :].astype(F32)
        for d in range(3):
            total = total + rrx[d, at, :].astype(F32)
        out_ref[at, :] = (mixed[at, :] + rms(total) * fgain_ref[...]).astype(BF16)
        return 0

    lax.fori_loop(0, half // strip, last, 0)

    for copy in started:
        copy.wait_send()

    @pl.when(k == 0)
    def _():
        for copy in kv_cond:
            copy.wait_send()

    @pl.when(k == 1)
    def _():
        for copy in relays:
            copy.wait_send()


def fused(sp, queries, keys, values, lambdas, head_gain, out_weight, residual, mix_gain,
          pre_gain, gate_weight, up_weight, down_weight, ffn_gain):
    rows, width = queries.shape[0], 128 * -(-(gate_weight.shape[1] // 128) // QUAD)
    half, model = residual.shape
    wrows = gate_weight.shape[0]
    vm = pl.BlockSpec(memory_space=pltpu.VMEM)
    V = pltpu.VMEM
    return pl.pallas_call(
        layer_kernel,
        out_shape=jax.ShapeDtypeStruct((half, model), BF16),
        in_specs=[vm, vm, vm, pl.BlockSpec(memory_space=pltpu.SMEM)] + [vm] * 9,
        out_specs=vm,
        scratch_shapes=[
            V((QUAD * rows, VD), BF16),
            V((sp * rows, VD), BF16),
            V((sp * rows, VD), BF16),
            V((sp * wrows, width), BF16),
            V((sp * wrows, width), BF16),
            V((sp * wrows, width), BF16),
            V((QUAD, 2 * rows, VD), BF16),
            V((QUAD, 1, 2 * rows), F32),
            V((QUAD, 1, 2 * rows), F32),
            V((QUAD, VD, 2 * rows), F32),
            V((QUAD, rows, VD), BF16),
            V((QUAD, rows, VD), BF16),
            V((half, model), BF16),
            V((half, model), BF16),
            V((half, model), F32),
            V((QUAD, rows, model), BF16),
            V((rows, model), BF16),
            V((QUAD, half, model), BF16),
            V((QUAD, half, model), BF16),
            V((QUAD, half, model), BF16),
            V((QUAD - 1, half, model), BF16),
            V((QUAD - 1, half, model), BF16),
            pltpu.SemaphoreType.DMA((96,)),
            pltpu.SemaphoreType.DMA((96,)),
            pltpu.SemaphoreType.DMA((6,)),
        ],
        compiler_params=pltpu.CompilerParams(
            collective_id=0, has_side_effects=True, vmem_limit_bytes=60 * 1024 * 1024
        ),
    )(
        queries, keys, values, lambdas, head_gain[None, :], out_weight, residual,
        mix_gain[None, :], pre_gain[None, :], gate_weight, up_weight, down_weight,
        ffn_gain[None, :],
    )


def solution(mesh):
    in_specs = (
        P("sp", "tp"),
        P("sp", "tp"),
        P("sp", "tp"),
        P("tp"),
        P(),
        P("tp", None),
        P(("sp", "tp"), None),
        P(),
        P(),
        P("sp", "tp"),
        P("sp", "tp"),
        P("sp", "tp"),
        P(),
    )
    out_specs = P(("sp", "tp"), None)
    sp, tp = mesh.shape["sp"], mesh.shape["tp"]
    body = functools.partial(fused, sp) if (sp, tp) == (16, 2) else on_device
    return jax.shard_map(
        body, mesh=mesh, in_specs=in_specs, out_specs=out_specs, check_vma=False
    )
```

```python
import functools
import math

import jax
import jax.numpy as jnp
from jax import lax
from jax.experimental import pallas as pl
from jax.experimental.pallas import tpu as pltpu
from jax.sharding import PartitionSpec as P

KD = 64
VD = 128


epsilon = 1e-06
negative = -1e30


def normalize(matrix, gain):
    return matrix * lax.rsqrt(jnp.mean(matrix * matrix, axis=-1, keepdims=True) + epsilon) * gain


def rounded(matrix):
    return lax.optimization_barrier(matrix.astype(jnp.bfloat16)).astype(jnp.float32)


def on_device(
    queries,
    keys,
    values,
    lambdas,
    head_gain,
    out_weight,
    residual,
    mix_gain,
    pre_gain,
    gate_weight,
    up_weight,
    down_weight,
    ffn_gain,
):
    rows = queries.shape[0]
    heads_dev = values.shape[1] // VD
    offset = lax.axis_index("sp") * rows
    scale = 1.0 / math.sqrt(KD)
    groups = [(queries, offset + jnp.arange(rows, dtype=jnp.int32))]
    grids = [
        (group_rows.reshape(group_rows.shape[0], heads_dev, 2, KD), group_pos)
        for group_rows, group_pos in groups
    ]
    initial = tuple(
        (
            (
                jnp.full((heads_dev, 2, grid.shape[0]), negative, jnp.float32),
                jnp.zeros((heads_dev, 2, grid.shape[0]), jnp.float32),
                jnp.zeros((heads_dev, 2, grid.shape[0], VD), jnp.float32),
            )
            for grid, _ in grids
        )
    )
    key_piece = lax.all_gather(keys, "sp", axis=0, tiled=True)
    value_piece = lax.all_gather(values, "sp", axis=0, tiled=True)
    count = key_piece.shape[0]
    block = math.gcd(count, max(256, 2048 // heads_dev))
    key_grid = key_piece.reshape(count, heads_dev, 2, KD)
    value_grid = value_piece.reshape(count, heads_dev, VD)
    results = []
    for (query_grid, query_pos), carried_group in zip(grids, initial):
        last_pos = query_pos[-1]

        def visit(index, carried, query_grid=query_grid, query_pos=query_pos, last_pos=last_pos):
            first = index * block

            def update(current):
                maxima, totals, accum = current
                key_block = lax.dynamic_slice_in_dim(key_grid, first, block, 0)
                value_block = lax.dynamic_slice_in_dim(value_grid, first, block, 0)
                scores = (
                    jnp.einsum(
                        "rhcd,nhcd->hcrn", query_grid, key_block, preferred_element_type=jnp.float32
                    )
                    * scale
                )
                key_pos = first + jnp.arange(block, dtype=jnp.int32)
                visible = key_pos[None, :] <= query_pos[:, None]
                block_max = jnp.max(jnp.where(visible, scores, negative), axis=-1)
                new_max = jnp.maximum(maxima, block_max)
                weights = jnp.where(visible, jnp.exp(scores - new_max[..., None]), 0.0)
                factor = jnp.exp(maxima - new_max)
                totals = totals * factor + jnp.sum(weights, axis=-1)
                accum = accum * factor[..., None] + jnp.einsum(
                    "hcrn,nhe->hcre",
                    weights.astype(jnp.bfloat16),
                    value_block,
                    preferred_element_type=jnp.float32,
                )
                return (new_max, totals, accum)

            return lax.cond(first <= last_pos, update, lambda current: current, carried)

        results.append(lax.fori_loop(0, count // block, visit, carried_group))
    states = tuple(results)
    totals = jnp.concatenate([state[1] for state in states], axis=2)
    accum = jnp.concatenate([state[2] for state in states], axis=2)
    ratio = accum / totals[..., None]
    attended = ratio[:, 0] - lambdas[:, None, None] * ratio[:, 1]
    heads_normed = normalize(attended, head_gain).astype(jnp.bfloat16)
    head_out = jnp.transpose(heads_normed, (1, 0, 2)).reshape(rows, heads_dev * VD)
    section = head_out
    projected = lax.psum_scatter(
        rounded(jnp.dot(section, out_weight, preferred_element_type=jnp.float32)).astype(
            jnp.bfloat16
        ),
        "tp",
        scatter_dimension=0,
        tiled=True,
    ).astype(jnp.float32)
    mixed = (residual.astype(jnp.float32) + normalize(projected, mix_gain)).astype(jnp.bfloat16)
    normed = normalize(mixed.astype(jnp.float32), pre_gain).astype(jnp.bfloat16)
    inputs = lax.all_gather(normed, "tp", axis=0, tiled=True)
    gate_sum = jnp.dot(
        inputs,
        lax.all_gather(gate_weight, "sp", axis=0, tiled=True),
        preferred_element_type=jnp.float32,
    )
    up_sum = jnp.dot(
        inputs,
        lax.all_gather(up_weight, "sp", axis=0, tiled=True),
        preferred_element_type=jnp.float32,
    )
    down_rows = lax.all_gather(down_weight, "sp", axis=0, tiled=True)
    hidden = (jax.nn.silu(gate_sum) * up_sum).astype(jnp.bfloat16)
    section = hidden
    ffn_out = lax.psum_scatter(
        rounded(
            lax.dot_general(
                section, down_rows, (((1,), (1,)), ((), ())), preferred_element_type=jnp.float32
            )
        ).astype(jnp.bfloat16),
        "tp",
        scatter_dimension=0,
        tiled=True,
    ).astype(jnp.float32)
    return (mixed.astype(jnp.float32) + normalize(ffn_out, ffn_gain)).astype(jnp.bfloat16)


MESH = pl.DeviceIdType.MESH
QUAD = 4
F32 = jnp.float32
BF16 = jnp.bfloat16


def nt_dot(a, b):
    return lax.dot_general(a, b, (((1,), (1,)), ((), ())), preferred_element_type=F32)


def tn_dot(a, b):
    return lax.dot_general(a, b, (((0,), (0,)), ((), ())), preferred_element_type=F32)


def rms(matrix):
    return matrix * lax.rsqrt(jnp.mean(matrix * matrix, axis=-1, keepdims=True) + epsilon)


def layer_kernel(
    q_ref, k_ref, v_ref, lam_ref, hgain_ref, ow_ref, res_ref, mgain_ref, pgain_ref,
    gw_ref, uw_ref, dw_ref, fgain_ref, out_ref,
    qbuf, kvbuf, wbuf, qz, m_st, l_st, acc_st, hs, ho,
    ptx, prx, mixed, xbuf, pbuf, ftx, frx, fown, rtx, rrx,
    send, recv, local,
):
    rows = q_ref.shape[0]
    half = rows // 2
    wrows = gw_ref.shape[0]
    width = wbuf.shape[1] // 3
    kbuf, vbuf = (kvbuf.at[:, i * VD : (i + 1) * VD] for i in range(2))
    gbuf, ubuf, dbuf = (wbuf.at[:, i * width : (i + 1) * width] for i in range(3))
    lanes = 128
    blocks = gw_ref.shape[1] // lanes
    per = width // lanes
    s = lax.axis_index("sp")
    c = lax.axis_index("tp")
    k = s // 8
    x = s % 2
    y = (s // 2) % 2

    def place(kk, qq):
        zz = qq // 2
        return (zz + kk * (1 - 2 * zz)) * 2 + qq % 2

    q = place(k, (s // 2) % 4)
    zl = q // 2

    def peer(d):
        return (zl if d < 2 else 1 - zl) * 2 + (y if d % 2 == 0 else 1 - y)

    def chip(kk, qq, xx):
        return kk * 8 + place(kk, qq) * 2 + xx

    sib = 1 - c
    qs = [peer(d) for d in range(4)]
    quad_dev = [(chip(k, qs[d], x), c) for d in range(4)]
    x_dev = (chip(k, q, 1 - x), c)
    k_dev = (chip(1 - k, q, x), c)
    sib_dev = (s, sib)

    barrier = pltpu.get_barrier_semaphore()
    partners = quad_dev[1:] + [x_dev, k_dev, sib_dev]
    for dev in partners:
        pl.semaphore_signal(barrier, inc=1, device_id=dev, device_id_type=MESH)
    pl.semaphore_wait(barrier, len(partners))

    def rc(src, dst, i, dev):
        return pltpu.make_async_remote_copy(
            src_ref=src, dst_ref=dst, send_sem=send.at[i], recv_sem=recv.at[i],
            device_id=dev, device_id_type=MESH,
        )

    def head_cols(qq):
        return pl.ds(pl.multiple_of(qq * lanes, lanes), lanes)

    def unit_start(qq):
        return jnp.minimum(qq * per, blocks - per)

    def unit_cols(qq):
        return pl.ds(pl.multiple_of(unit_start(qq) * lanes, lanes), width)

    def kv_rows(ss):
        return pl.ds(pl.multiple_of(ss * rows, rows), rows)

    def w_rows(ss):
        return pl.ds(pl.multiple_of(ss * wrows, wrows), wrows)

    started = []

    def go(copy):
        copy.start()
        started.append(copy)

    me = s
    kv = [kbuf, vbuf]
    ws = [gbuf, ubuf, dbuf]
    own = []
    for i, (src, dst, at, cols) in enumerate(
        [
            (q_ref, qbuf, kv_rows(place(k, q)), head_cols(q)),
            (k_ref, kbuf, kv_rows(me), head_cols(q)),
            (v_ref, vbuf, kv_rows(me), head_cols(q)),
            (gw_ref, gbuf, w_rows(me), unit_cols(q)),
            (uw_ref, ubuf, w_rows(me), unit_cols(q)),
            (dw_ref, dbuf, w_rows(me), unit_cols(q)),
        ]
    ):
        cp = pltpu.make_async_copy(src.at[:, cols], dst.at[at, :], local.at[i])
        cp.start()
        own.append(cp)
    for d in (1, 2, 3):
        for a, (src, dst) in enumerate([(k_ref, kbuf), (v_ref, vbuf), (q_ref, qbuf)]):
            slot = dst.at[kv_rows(me if a < 2 else place(k, q)), :]
            go(rc(src.at[:, head_cols(qs[d])], slot, (d - 1) * 6 + a, quad_dev[d]))
    for d in (1, 2, 3):
        for a, (src, dst) in enumerate([(gw_ref, gbuf), (uw_ref, ubuf), (dw_ref, dbuf)]):
            go(rc(src.at[:, unit_cols(qs[d])], dst.at[w_rows(me), :], (d - 1) * 6 + 3 + a, quad_dev[d]))
    for cp in own:
        cp.wait()

    X0, K0, R0 = 18, 38, 58
    kv_cond = []

    def kvslot(ss):
        return kvbuf.at[kv_rows(ss), :]

    def allslot(ss):
        return wbuf.at[w_rows(ss), :]

    def kslot(a, ss):
        return kv[a].at[kv_rows(ss), :]

    def wslot(a, ss):
        return ws[a].at[w_rows(ss), :]

    def forward_kv(d):
        ss = chip(k, qs[d], x)
        if d > 0:
            for a in range(2):
                slot = kslot(a, ss)
                rc(slot, slot, (d - 1) * 6 + a, quad_dev[d]).wait_recv()
        slot = kvslot(ss)
        copy = rc(slot, slot, K0 + d * 5, k_dev)
        kv_cond.append(copy)

        @pl.when(k == 0)
        def _(copy=copy):
            copy.start()

        go(rc(slot, slot, X0 + d * 5, x_dev))

    def forward_w(d):
        ss = chip(k, qs[d], x)
        if d > 0:
            for a in range(3):
                slot = wslot(a, ss)
                rc(slot, slot, (d - 1) * 6 + 3 + a, quad_dev[d]).wait_recv()
        slot = allslot(ss)
        go(rc(slot, slot, K0 + d * 5 + 2, k_dev))
        go(rc(slot, slot, X0 + d * 5 + 2, x_dev))

    forward_kv(0)
    forward_w(0)
    for d in (1, 2, 3):
        forward_kv(d)
    for d in (1, 2, 3):
        forward_w(d)
    for d in (1, 2, 3):
        slot = qbuf.at[kv_rows(place(k, qs[d])), :]
        rc(slot, slot, (d - 1) * 6 + 2, quad_dev[d]).wait_recv()
    for d in range(4):
        for a in range(1):
            slot = kvslot(chip(k, qs[d], 1 - x))
            rc(slot, slot, X0 + d * 5 + a, x_dev).wait_recv()

    span = 2 * rows
    lane = lax.broadcasted_iota(jnp.int32, (rows, lanes), 1)
    for j in range(4):
        piece = qbuf[j * rows : (j + 1) * rows, :].astype(F32) * (1.0 / math.sqrt(KD))
        qz[j, :rows, :] = jnp.where(lane < KD, piece, 0.0).astype(BF16)
        qz[j, rows:, :] = jnp.where(lane < KD, 0.0, piece).astype(BF16)

    def pair_rows(p):
        return pl.ds(pl.multiple_of(p * span, span), span)

    def update(j, p, carry):
        m, l, acc = carry
        sc = nt_dot(kbuf[pair_rows(p), :], qz[j])
        new = jnp.maximum(m, jnp.max(sc, axis=0, keepdims=True))
        e = jnp.exp(sc - new)
        f = jnp.exp(m - new)
        l = l * f + jnp.sum(e, axis=0, keepdims=True)
        acc = acc * f + tn_dot(vbuf[pair_rows(p), :], e.astype(BF16))
        return new, l, acc

    def chunk_a(j, _):
        p = 4 * k + j
        sc = nt_dot(kbuf[pair_rows(p), :], qz[j])
        key_pos = lax.broadcasted_iota(jnp.int32, sc.shape, 0)
        query_pos = x * rows + lax.broadcasted_iota(jnp.int32, sc.shape, 1) % rows
        sc = jnp.where(key_pos <= query_pos, sc, negative)
        m = jnp.max(sc, axis=0, keepdims=True)
        e = jnp.exp(sc - m)
        l = jnp.sum(e, axis=0, keepdims=True)
        acc = tn_dot(vbuf[pair_rows(p), :], e.astype(BF16))
        m, l, acc = lax.fori_loop(0, j, lambda i, carry: update(j, 4 * k + i, carry), (m, l, acc))
        m_st[j], l_st[j], acc_st[j] = m, l, acc
        return 0

    relays = []
    for d in range(4):
        for a in range(1):
            slot = kvslot(chip(1 - k, qs[d], x))
            relays.append(rc(slot, slot, R0 + d * 5 + a, x_dev))

    def relay_kv(d):
        @pl.when(k == 1)
        def _():
            for a in range(1):
                slot = kvslot(chip(1 - k, qs[d], x))
                rc(slot, slot, K0 + d * 5 + a, k_dev).wait_recv()
                relays[d].start()

    def chunk_b(d):
        @pl.when(k == 1)
        def _():
            for a in range(1):
                slot = kvslot(chip(1 - k, qs[d], 1 - x))
                rc(slot, slot, R0 + d * 5 + a, x_dev).wait_recv()

            def one(j, _):
                m_st[j], l_st[j], acc_st[j] = update(j, qs[d], (m_st[j], l_st[j], acc_st[j]))
                return 0

            lax.fori_loop(0, 4, one, 0)

    lax.fori_loop(0, 3, chunk_a, 0)
    relay_kv(0)
    lax.fori_loop(3, 4, chunk_a, 0)
    relay_kv(1)
    chunk_b(0)
    relay_kv(2)
    chunk_b(1)
    relay_kv(3)
    chunk_b(2)
    chunk_b(3)

    lam = lam_ref[q]

    def finish(j, _):
        ratio = acc_st[j] / l_st[j]
        att = (ratio[:, :rows] - lam * ratio[:, rows:]).T
        hs[j] = (rms(att) * hgain_ref[...]).astype(BF16)
        return 0

    lax.fori_loop(0, 4, finish, 0)
    H0 = 78
    for d in (3, 1, 2):
        go(rc(hs.at[place(k, qs[d])], ho.at[q], H0 + d - 1, quad_dev[d]))
    ho[q] = hs[place(k, q)]

    def relay_w(d):
        for a in range(1):
            slot = allslot(chip(1 - k, qs[d], x))
            rc(slot, slot, K0 + d * 5 + 2 + a, k_dev).wait_recv()
            go(rc(slot, slot, R0 + d * 5 + 2 + a, x_dev))

    relay_w(0)
    for d in (1, 2, 3):
        rc(ho.at[qs[d]], ho.at[qs[d]], H0 + d - 1, quad_dev[d]).wait_recv()

    def head_rows(cc):
        at = pl.ds(pl.multiple_of(cc * half, half), half)
        return jnp.concatenate([ho[j, at, :] for j in range(4)], axis=1)

    theirs = head_rows(sib)
    ptx[...] = jnp.dot(theirs, ow_ref[...], preferred_element_type=F32).astype(BF16)
    P0 = 81
    go(rc(ptx, prx, P0, sib_dev))
    relay_w(1)
    mixed[...] = jnp.dot(head_rows(c), ow_ref[...], preferred_element_type=F32)
    rc(prx, prx, P0, sib_dev).wait_recv()

    strip = 16

    def pass_rows(d):
        slot = xbuf.at[qs[d], core_rows[0], :]
        rc(slot, slot, A0 + d - 1, quad_dev[d]).wait_recv()
        go(rc(slot, slot, S0 + d, sib_dev))

    def mix(i, _):
        at = pl.ds(pl.multiple_of(i * strip, strip), strip)
        total = mixed[at, :].astype(BF16).astype(F32) + prx[at, :].astype(F32)
        mx = (res_ref[at, :].astype(F32) + rms(total) * mgain_ref[...]).astype(BF16).astype(F32)
        mixed[at, :] = mx
        xbuf[q, pl.ds(pl.multiple_of(c * half + i * strip, strip), strip), :] = (
            rms(mx) * pgain_ref[...]
        ).astype(BF16)
        return 0

    lax.fori_loop(0, half // strip, mix, 0)

    A0, S0 = 82, 85
    core_rows = [pl.ds(pl.multiple_of(cc * half, half), half) for cc in (c, sib)]
    mine = xbuf.at[q, core_rows[0], :]
    for d in (3, 1, 2):
        go(rc(mine, mine, A0 + d - 1, quad_dev[d]))
    go(rc(mine, mine, S0, sib_dev))

    for d in (1, 2):
        relay_w(d + 1)
        pass_rows(d)
    pass_rows(3)
    for a in range(1):
        for d in range(4):
            slot = allslot(chip(k, qs[d], 1 - x))
            rc(slot, slot, X0 + d * 5 + 2 + a, x_dev).wait_recv()
        for d in range(4):
            slot = allslot(chip(1 - k, qs[d], 1 - x))
            rc(slot, slot, R0 + d * 5 + 2 + a, x_dev).wait_recv()

    F0, C0 = 89, 93
    fresh = (q * per - unit_start(q)) * lanes
    unit = lax.broadcasted_iota(jnp.int32, (rows, width), 1)

    def summed(d):
        slot = frx.at[d]
        rc(slot, slot, F0 + d, sib_dev).wait_recv()
        total = fown[d].astype(F32) + frx[d].astype(F32)
        if d == 0:
            fown[0] = total.astype(BF16)
        else:
            rtx[d - 1] = total.astype(BF16)
            go(rc(rtx.at[d - 1], rrx.at[d - 1], C0 + d - 1, quad_dev[d]))

    order = (3, 1, 2, 0)
    for n, d in enumerate(order):
        slot = xbuf.at[qs[d], core_rows[1], :]
        rc(slot, slot, S0 + d, sib_dev).wait_recv()
        rows_in = xbuf[qs[d]]
        gate = jnp.dot(rows_in, gbuf[...], preferred_element_type=F32)
        up = jnp.dot(rows_in, ubuf[...], preferred_element_type=F32)
        hid = gate / (1.0 + jnp.exp(-gate)) * up
        hid = jnp.where(unit >= fresh, hid, 0.0).astype(BF16)
        pbuf[...] = nt_dot(hid, dbuf[...]).astype(BF16)
        ftx[d] = pbuf[core_rows[1], :]
        fown[d] = pbuf[core_rows[0], :]
        go(rc(ftx.at[d], frx.at[d], F0 + d, sib_dev))
        if n > 0:
            summed(order[n - 1])
    summed(order[-1])
    for d in (1, 2, 3):
        slot = rrx.at[d - 1]
        rc(slot, slot, C0 + d - 1, quad_dev[d]).wait_recv()

    def last(i, _):
        at = pl.ds(pl.multiple_of(i * strip, strip), strip)
        total = fown[0, at, :].astype(F32)
        for d in range(3):
            total = total + rrx[d, at, :].astype(F32)
        out_ref[at, :] = (mixed[at, :] + rms(total) * fgain_ref[...]).astype(BF16)
        return 0

    lax.fori_loop(0, half // strip, last, 0)

    for copy in started:
        copy.wait_send()

    @pl.when(k == 0)
    def _():
        for copy in kv_cond:
            copy.wait_send()

    @pl.when(k == 1)
    def _():
        for copy in relays:
            copy.wait_send()


def fused(sp, queries, keys, values, lambdas, head_gain, out_weight, residual, mix_gain,
          pre_gain, gate_weight, up_weight, down_weight, ffn_gain):
    rows, width = queries.shape[0], 128 * -(-(gate_weight.shape[1] // 128) // QUAD)
    half, model = residual.shape
    wrows = gate_weight.shape[0]
    vm = pl.BlockSpec(memory_space=pltpu.VMEM)
    V = pltpu.VMEM
    return pl.pallas_call(
        layer_kernel,
        out_shape=jax.ShapeDtypeStruct((half, model), BF16),
        in_specs=[vm, vm, vm, pl.BlockSpec(memory_space=pltpu.SMEM)] + [vm] * 9,
        out_specs=vm,
        scratch_shapes=[
            V((QUAD * rows, VD), BF16),
            V((sp * rows, 2 * VD), BF16),
            V((sp * wrows, 3 * width), BF16),
            V((QUAD, 2 * rows, VD), BF16),
            V((QUAD, 1, 2 * rows), F32),
            V((QUAD, 1, 2 * rows), F32),
            V((QUAD, VD, 2 * rows), F32),
            V((QUAD, rows, VD), BF16),
            V((QUAD, rows, VD), BF16),
            V((half, model), BF16),
            V((half, model), BF16),
            V((half, model), F32),
            V((QUAD, rows, model), BF16),
            V((rows, model), BF16),
            V((QUAD, half, model), BF16),
            V((QUAD, half, model), BF16),
            V((QUAD, half, model), BF16),
            V((QUAD - 1, half, model), BF16),
            V((QUAD - 1, half, model), BF16),
            pltpu.SemaphoreType.DMA((96,)),
            pltpu.SemaphoreType.DMA((96,)),
            pltpu.SemaphoreType.DMA((6,)),
        ],
        compiler_params=pltpu.CompilerParams(
            collective_id=0, has_side_effects=True, vmem_limit_bytes=60 * 1024 * 1024
        ),
    )(
        queries, keys, values, lambdas, head_gain[None, :], out_weight, residual,
        mix_gain[None, :], pre_gain[None, :], gate_weight, up_weight, down_weight,
        ffn_gain[None, :],
    )


def solution(mesh):
    in_specs = (
        P("sp", "tp"),
        P("sp", "tp"),
        P("sp", "tp"),
        P("tp"),
        P(),
        P("tp", None),
        P(("sp", "tp"), None),
        P(),
        P(),
        P("sp", "tp"),
        P("sp", "tp"),
        P("sp", "tp"),
        P(),
    )
    out_specs = P(("sp", "tp"), None)
    sp, tp = mesh.shape["sp"], mesh.shape["tp"]
    body = functools.partial(fused, sp) if (sp, tp) == (16, 2) else on_device
    return jax.shard_map(
        body, mesh=mesh, in_specs=in_specs, out_specs=out_specs, check_vma=False
    )
```
